32 devices in a mesh: kv: 16 (over z, y, x), tp: 2 (over core).
Axes of the slice: x: 2, y: 2, z: 4, core: 2. Of those that a mesh axis runs over, the one named last changes fastest.
Arguments:
- tokens: bfloat16 [8, 2048, 2048], P(None, 'kv'), may hold values from -32 to 32, as said below
- w_query: bfloat16 [2048, 1024], P(None, 'tp'), may hold values from -0.125 to 0.125
- w_key: bfloat16 [2048, 512], P(None, 'tp'), may hold values from -0.125 to 0.125
- w_value: bfloat16 [2048, 512], P(None, 'tp'), may hold values from -0.125 to 0.125
- w_output: bfloat16 [1024, 2048], P(None, 'tp'), may hold values from -3 to 3
- chosen: int32 [8, 16, 32], P(None, 'kv'), may hold values from -1 to 15, as said below
- lengths: int32 [8], replicated, may hold values from 1 to 2048, 5632 in all
Outputs:
- mixed: bfloat16 [8, 2048, 2048], P(None, 'kv', 'tp')
The draws below stay inside these ranges and needn't reach their ends.
Inputs may be any that keep to these rules, and one draw needn't show every extreme that they name: chosen[s, b] lists distinct blocks of sequence s, none above b; its first entry is b; entries after the named ones are -1. For b >= 1 and each c < b, at most 4 of the 8 lists chosen[:, b] name block c, and exactly 4 of them name block b - 1. lengths[s] is the number of live positions of sequence s; the largest is 2048. `tokens`: activations of order one; some rows may be much larger.
All inputs are finite; a program needn't handle non-finite values.
Results may differ from the reference program's by a relative error of at most 0.012.
The reference program's roundings to bfloat16 on the way count: a program that leaves them out, or rounds other values in their place, can miss the bound.
Values may be sent and summed in bfloat16 or wider, within the bound.
A program may use at most 128 MiB of HBM per device.

```python
import math
import jax
import jax.numpy as jnp
import numpy as np
from jax import lax

D = 2048
HEADS = 16
KV_HEADS = 8
HEAD_DIM = 64
BLK = 128
SEL = 32
SEQS = 8
CAP = 4
SEQ_LEN = 2048
BLOCKS_PER_SEQ = 16


def draw_tokens(key, part):
    shape = (SEQS, SEQ_LEN, D)
    return jnp.clip(jax.random.normal(key, shape, jnp.float32), -6.0, 6.0).astype(jnp.bfloat16)


def draw_chosen(key, part):
    key_allow, key_ordering = jax.random.split(jax.random.fold_in(key, 7))
    owners = jnp.arange(BLOCKS_PER_SEQ, dtype=jnp.int32)
    raw_scores = jax.random.randint(key_allow, (BLOCKS_PER_SEQ, BLOCKS_PER_SEQ, SEQS), 0, 1 << 20) * SEQS + jnp.arange(SEQS, dtype=jnp.int32)
    beaten = jnp.sum((raw_scores[:, :, None, :] > raw_scores[:, :, :, None]).astype(jnp.int32), axis=-1)
    permitted = beaten < CAP
    shard_member = owners[:, None]
    block_keeper = owners[None, :]
    earlier = block_keeper < shard_member
    candidate = earlier[None, :, :] & jnp.transpose(permitted, (2, 0, 1))
    own_block = (block_keeper == shard_member)[None, :, :]
    extra_score = jnp.where(block_keeper == shard_member, 4, jnp.where(block_keeper == shard_member - 1, 3, jnp.where(block_keeper == shard_member - BLOCKS_PER_SEQ // 2, 2, jnp.where(block_keeper == 0, 1, 0))))
    random_jitter = jax.random.randint(key_ordering, (SEQS, BLOCKS_PER_SEQ, BLOCKS_PER_SEQ), 0, 1 << 16)
    block_precedence = (extra_score[None, :, :] * (1 << 20) + random_jitter) * BLOCKS_PER_SEQ + block_keeper[None, :, :]
    block_precedence = jnp.where(candidate | own_block, block_precedence, -1)
    slot_count = min(SEL, BLOCKS_PER_SEQ)
    ranked, _ = lax.top_k(block_precedence, slot_count)
    picked = jnp.where(ranked >= 0, ranked % BLOCKS_PER_SEQ, -1)
    if slot_count < SEL:
        picked = jnp.concatenate([picked, jnp.full((SEQS, BLOCKS_PER_SEQ, SEL - slot_count), -1, jnp.int32)], axis=-1)
    return picked.astype(jnp.int32)


def block_scale(stream_key, dims, shards, smallest, largest):
    factor_of, own = 1.0, jax.random.fold_in(stream_key, 6)
    for axis_at, shards_of in shards:
        draws = jnp.exp(jax.random.uniform(jax.random.fold_in(own, axis_at), (shards_of,), jnp.float32, smallest / len(shards), largest / len(shards)))
        factor_of = factor_of * jnp.repeat(draws, dims[axis_at] // shards_of).reshape([-1 if axis == axis_at else 1 for axis in range(len(dims))])
    return factor_of


def split_up(number_of, total, reach, slope):
    loads = [(1 << 20) // math.isqrt(standing ** slope) + 1 for standing in range(2, number_of + 1)]
    surplus, given = total - reach - (number_of - 1), [1] * (number_of - 1)
    while surplus > 0:
        candidates = [i for i in range(number_of - 1) if given[i] < reach]
        pool, left = sum([loads[i] for i in candidates]), surplus
        for i in candidates:
            addition = min(reach - given[i], max(1, left * loads[i] // pool), surplus)
            given[i] = given[i] + addition
            surplus = surplus - addition
    return np.array([reach] + given)


def ragged(rng, amount, total, limit, skew):
    if amount == 2:
        one = jax.random.randint(rng, (), max(1, total - limit), min(limit, total - 1) + 1)
        return jnp.stack([one, total - one])
    sizes = jnp.asarray(split_up(amount, total, limit, skew), jnp.int32)
    couples = (amount - 1) // 2
    donor, receiver = sizes[1:1 + 2 * couples:2], sizes[2:2 + 2 * couples:2]
    margin = jnp.minimum(donor - 1, limit - receiver)
    shifted = jax.random.randint(jax.random.fold_in(rng, 1), (couples,), 0, 1 << 20) % (margin + 1)
    sizes = sizes.at[1:1 + 2 * couples:2].set(donor - shifted).at[2:2 + 2 * couples:2].set(receiver + shifted)
    return sizes[jax.random.permutation(jax.random.fold_in(rng, 2), amount)]


def bell_draw(key, extent, spread, reach, cuts=(), kind=jnp.bfloat16):
    gain = block_scale(key, extent, cuts, -0.22, 0.18) if cuts else 1.0
    drawn = jax.random.normal(key, extent, jnp.float32) * spread * gain
    return jnp.minimum(jnp.maximum(drawn, -reach), reach).astype(kind)


def setup_inputs(seed: int = 0) -> dict:
    arg_keys = jax.random.split(jax.random.key(seed), 8)
    return {
        "tokens": draw_tokens(jax.random.fold_in(arg_keys[7], 71), 0),
        "w_query": bell_draw(arg_keys[1], (D, HEADS * HEAD_DIM), D ** -0.5, 0.125, ((1, 2),)),
        "w_key": bell_draw(arg_keys[2], (D, KV_HEADS * HEAD_DIM), D ** -0.5, 0.125, ((1, 2),)),
        "w_value": bell_draw(arg_keys[3], (D, KV_HEADS * HEAD_DIM), D ** -0.5, 0.125, ((1, 2),)),
        "w_output": bell_draw(arg_keys[4], (HEADS * HEAD_DIM, D), 0.5, 3.0, ((1, 2),)),
        "chosen": draw_chosen(jax.random.fold_in(arg_keys[7], 71), 0),
        "lengths": ragged(arg_keys[6], SEQS, SEQ_LEN + (SEQS - 1) * SEQ_LEN // 4, SEQ_LEN, 2).astype(jnp.int32),
    }


def attend_block(query_rows, key_seq, value_seq, pick_row, first_pos, length):
    clipped = jnp.maximum(pick_row, 0)
    key_rows = key_seq[clipped].reshape(SEL * BLK, KV_HEADS, HEAD_DIM).astype(jnp.float32)
    value_rows = value_seq[clipped].reshape(SEL * BLK, KV_HEADS, HEAD_DIM).astype(jnp.float32)
    grouped = query_rows.reshape(BLK, KV_HEADS, HEADS // KV_HEADS, HEAD_DIM).astype(jnp.float32)
    scores = jnp.einsum("qkgd,nkd->kgqn", grouped, key_rows) * HEAD_DIM ** -0.5
    query_pos = first_pos + jnp.arange(BLK, dtype=jnp.int32)
    key_pos = (pick_row[:, None] * BLK + jnp.arange(BLK, dtype=jnp.int32)[None, :]).reshape(-1)
    listed = jnp.repeat(pick_row >= 0, BLK)
    allowed = listed[None, :] & (key_pos[None, :] <= query_pos[:, None]) & (key_pos[None, :] < length)
    masked = jnp.where(allowed, scores, -1e30)
    row_max = jnp.max(masked, axis=-1, keepdims=True)
    exponent = jnp.exp(masked - row_max)
    weights = (exponent / jnp.sum(exponent, axis=-1, keepdims=True)).astype(jnp.bfloat16)
    weights = lax.optimization_barrier(weights).astype(jnp.float32)
    mixed_heads = jnp.einsum("kgqn,nkd->qkgd", weights, value_rows)
    live_rows = (query_pos < length)[:, None, None, None]
    return jnp.where(live_rows, mixed_heads, 0.0).astype(jnp.bfloat16).reshape(BLK, HEADS * HEAD_DIM)


def reference(tokens, w_query, w_key, w_value, w_output, chosen, lengths):
    flat_rows = tokens.reshape(SEQS * SEQ_LEN, D)
    queries = lax.optimization_barrier(jnp.dot(flat_rows, w_query, preferred_element_type=jnp.float32).astype(jnp.bfloat16))
    key_proj = lax.optimization_barrier(jnp.dot(flat_rows, w_key, preferred_element_type=jnp.float32).astype(jnp.bfloat16))
    value_proj = lax.optimization_barrier(jnp.dot(flat_rows, w_value, preferred_element_type=jnp.float32).astype(jnp.bfloat16))
    queries = queries.reshape(SEQS, BLOCKS_PER_SEQ, BLK, HEADS * HEAD_DIM)
    key_proj = key_proj.reshape(SEQS, BLOCKS_PER_SEQ, BLK, KV_HEADS, HEAD_DIM)
    value_proj = value_proj.reshape(SEQS, BLOCKS_PER_SEQ, BLK, KV_HEADS, HEAD_DIM)

    def one_seq(packed):
        query_seq, key_seq, value_seq, pick_seq, length = packed

        def one_block(inner_pack):
            query_rows, pick_row, block_id = inner_pack
            return attend_block(query_rows, key_seq, value_seq, pick_row, block_id * BLK, length)

        return lax.map(one_block, (query_seq, pick_seq, jnp.arange(BLOCKS_PER_SEQ, dtype=jnp.int32)))

    attended = lax.map(one_seq, (queries, key_proj, value_proj, chosen, lengths))
    mixed = jnp.dot(attended.reshape(SEQS * SEQ_LEN, HEADS * HEAD_DIM), w_output, preferred_element_type=jnp.float32)
    return mixed.astype(jnp.bfloat16).reshape(SEQS, SEQ_LEN, D)
```

```python
import functools

import jax
import jax.numpy as jnp
from jax import lax
from jax.experimental import pallas as pl
from jax.experimental.pallas import tpu as pltpu
from jax.sharding import PartitionSpec as P

HEADS = 16
KV_HEADS = 8
HEAD_DIM = 64
CAP = 4
LANES = 128
MESH = pl.DeviceIdType.MESH
VMEM_LIMIT = 60 * 1024 * 1024


def blocks_to(dest, n, block_len, cap):
    seq_len = n * block_len
    spare = seq_len * 7 // 4
    count = jnp.int32(1)
    for k in range(1, cap):
        count = count + (k * (dest * block_len + 1) <= spare).astype(jnp.int32)
    return count


def greet(axis, me, n):
    barrier = pltpu.get_barrier_semaphore()
    for k in range(1, n):
        pl.semaphore_signal(
            barrier, inc=1, device_id={axis: lax.rem(me + k, n)}, device_id_type=MESH
        )
    return barrier


def project_kernel(
    n, steps, x_ref, wq_ref, wk_ref, wv_ref, chosen_ref, len_ref,
    q_ref, kv_ref, rank_ref, got_ref, incoming_ref, req_ref, send_sem, recv_sem,
):
    step = pl.program_id(0)
    me = lax.axis_index("kv")
    seqs, slots = chosen_ref.shape
    seqs_now, block_len, width = x_ref.shape
    kw = wk_ref.shape[1]

    def request_copy(dest, slot, k=0):
        return pltpu.make_async_remote_copy(
            src_ref=req_ref,
            dst_ref=incoming_ref.at[slot],
            send_sem=send_sem.at[k],
            recv_sem=recv_sem.at[slot],
            device_id={"kv": dest},
            device_id_type=MESH,
        )

    @pl.when(step == 0)
    def _():
        greet("kv", me, n)
        owner = lax.broadcasted_iota(jnp.int32, (seqs, LANES), 1)
        picked = chosen_ref[...]
        wanted = jnp.zeros((seqs, LANES), jnp.int32)
        for j in range(slots):
            wanted = wanted | (picked[:, j : j + 1] == owner).astype(jnp.int32)
        live = len_ref[...] > me * block_len
        wanted = jnp.where(live & (owner < me), wanted, 0)
        count = jnp.zeros((1, LANES), jnp.int32)
        rows = [jnp.zeros((1, LANES), jnp.int32) for _ in range(CAP)]
        ranks = []
        for s in range(seqs):
            hit = wanted[s : s + 1]
            ranks.append(count)
            for r in range(CAP):
                rows[r] = jnp.where((hit > 0) & (count == r), s, rows[r])
            count = count + hit
        rank_ref[...] = jnp.concatenate(ranks, axis=0)
        fill = [jnp.zeros((8 - CAP, LANES), jnp.int32)]
        req_ref[...] = jnp.concatenate(rows + fill, axis=0)
        incoming_ref[me] = jnp.zeros((8, LANES), jnp.int32)

    rows = x_ref[...].reshape(seqs_now * block_len, width)
    scale = HEAD_DIM ** (-0.5)

    def project(w_ref):
        out = jnp.dot(rows, w_ref[...], preferred_element_type=jnp.float32).astype(jnp.bfloat16)
        return out.reshape(seqs_now, block_len, -1)

    q_ref[...] = project(wq_ref) * jnp.bfloat16(scale)
    kv_ref[:, :, :kw] = project(wk_ref)
    kv_ref[:, :, kw:] = project(wv_ref)

    @pl.when(step == 0)
    def _():
        pl.semaphore_wait(pltpu.get_barrier_semaphore(), n - 1)
        for k in range(1, n):
            request_copy(lax.rem(me + k, n), me, k).start()

    @pl.when(step == steps - 1)
    def _():
        for k in range(1, n):
            request_copy(lax.rem(me + k, n), me, k).wait_send()
        for k in range(1, n):
            other = lax.rem(me + k, n)
            request_copy(other, other).wait_recv()
        got_ref[...] = incoming_ref[...]


def exchange_kernel(n, idx_ref, kv_ref, arrived_ref, pack_ref, send_sem, recv_sem):
    me = lax.axis_index("kv")
    block_len = kv_ref.shape[1]
    barrier = greet("kv", me, n)

    def copy(k, dest, slot, blocks):
        return pltpu.make_async_remote_copy(
            src_ref=pack_ref.at[k, pl.ds(0, blocks)],
            dst_ref=arrived_ref.at[slot, pl.ds(0, blocks)],
            send_sem=send_sem.at[k],
            recv_sem=recv_sem.at[slot],
            device_id={"kv": dest},
            device_id_type=MESH,
        )

    def each_send(k, act):
        dest = me + k
        count = blocks_to(dest, n, block_len, CAP)
        for blocks in range(1, CAP + 1):
            @pl.when((dest < n) & (count == blocks))
            def _():
                act(copy(k, dest, me, blocks))

    for k in range(1, n + 1):
        if k < n:
            @pl.when(me + k < n)
            def _():
                for r in range(CAP):
                    pack_ref[k, r] = kv_ref[idx_ref[(me + k) * CAP + r]]
        if k == 2:
            pl.semaphore_wait(barrier, n - 1)
        if k >= 2:
            each_send(k - 1, lambda c: c.start())
    for k in range(1, n):
        each_send(k, lambda c: c.wait_send())
    mine = blocks_to(me, n, block_len, CAP)
    for k in range(1, n):
        for blocks in range(1, CAP + 1):
            @pl.when((me - k >= 0) & (mine == blocks))
            def _():
                copy(k, me - k, me - k, blocks).wait_recv()


def attend_kernel(
    len_ref, pick_ref, rank_ref, q_ref, kv_ref, arr_ref, out_ref,
    qs_ref, s_ref, m_ref, l_ref, acc_ref,
):
    s = pl.program_id(0)
    me = lax.axis_index("kv")
    block_len, qw = q_ref.shape[1:]
    kw = kv_ref.shape[2] // 2
    w = min(LANES, kw)
    tiles, per_tile = kw // w, w // HEAD_DIM
    group = HEADS // KV_HEADS
    heads = group * per_tile
    rows = heads * block_len
    slots = pick_ref.shape[1]
    length = len_ref[s]
    live = length > me * block_len

    @pl.when(jnp.logical_not(live))
    def _():
        out_ref[...] = jnp.zeros(out_ref.shape, out_ref.dtype)

    @pl.when(live)
    def _():
        count = jnp.int32(0)
        for j in range(slots):
            count = count + (pick_ref[s, j] >= 0).astype(jnp.int32)
        zero = jnp.zeros((block_len, HEAD_DIM), jnp.bfloat16)
        for t in range(tiles):
            for i in range(heads):
                h = t * heads + i
                own = q_ref[0, :, h * HEAD_DIM : (h + 1) * HEAD_DIM]
                parts = [own if i // group == p else zero for p in range(per_tile)]
                qs_ref[t, i * block_len : (i + 1) * block_len, :] = jnp.concatenate(parts, axis=1)

        def score(t, keys):
            return lax.dot_general(
                qs_ref[t], keys, (((1,), (1,)), ((), ())), preferred_element_type=jnp.float32
            )

        key_at = lax.broadcasted_iota(jnp.int32, (heads, block_len, block_len), 2)
        row_at = lax.broadcasted_iota(jnp.int32, (heads, block_len, block_len), 1)
        causal = (key_at <= row_at).reshape(rows, block_len)
        for t in range(tiles):
            first = jnp.where(causal, score(t, kv_ref[0, :, t * w : (t + 1) * w]), -1e30)
            s_ref[0, t] = first
            m_ref[t] = first

        def score_slot(j, carry):
            c = pick_ref[s, j]
            r = rank_ref[s, c]
            for t in range(tiles):
                got = score(t, arr_ref[c, r, :, t * w : (t + 1) * w])
                s_ref[j, t] = got
                m_ref[t] = jnp.maximum(m_ref[t], got)
            return carry

        lax.fori_loop(1, count, score_slot, 0)
        for t in range(tiles):
            top = jnp.max(m_ref[t], axis=1, keepdims=True)
            m_ref[t] = jnp.broadcast_to(top, (rows, block_len))
            p = jnp.exp(s_ref[0, t] - top)
            l_ref[t] = p
            acc_ref[t] = jnp.dot(
                p.astype(jnp.bfloat16),
                kv_ref[0, :, kw + t * w : kw + (t + 1) * w],
                preferred_element_type=jnp.float32,
            )

        def value_slot(j, carry):
            c = pick_ref[s, j]
            r = rank_ref[s, c]
            for t in range(tiles):
                p = jnp.exp(s_ref[j, t] - m_ref[t])
                l_ref[t] = l_ref[t] + p
                acc_ref[t] = acc_ref[t] + jnp.dot(
                    p.astype(jnp.bfloat16),
                    arr_ref[c, r, :, kw + t * w : kw + (t + 1) * w],
                    preferred_element_type=jnp.float32,
                )
            return carry

        lax.fori_loop(1, count, value_slot, 0)
        at = me * block_len + lax.broadcasted_iota(jnp.int32, (block_len, w), 0)
        for t in range(tiles):
            total = jnp.sum(l_ref[t], axis=1, keepdims=True)
            done = acc_ref[t] / total
            for i in range(heads):
                h = t * heads + i
                part = done[i * block_len : (i + 1) * block_len]
                part = jnp.where(at < length, part, 0.0).astype(jnp.bfloat16)
                lane = (i // group) * HEAD_DIM
                out_ref[0, :, h * HEAD_DIM : (h + 1) * HEAD_DIM] = part[:, lane : lane + HEAD_DIM]


def mix_kernel(tp, att_ref, w_ref, out_ref, held_ref, acc_ref, send_sem, recv_sem):
    me = lax.axis_index("tp")
    seqs, block_len, hw = att_ref.shape
    chunk = 2
    barrier = greet("tp", me, tp)
    pl.semaphore_wait(barrier, tp - 1)

    def copy(k, dest):
        return pltpu.make_async_remote_copy(
            src_ref=att_ref,
            dst_ref=held_ref.at[k - 1],
            send_sem=send_sem.at[k - 1],
            recv_sem=recv_sem.at[k - 1],
            device_id={"tp": dest},
            device_id_type=MESH,
        )

    for k in range(1, tp):
        copy(k, lax.rem(me + k, tp)).start()

    def term(rows, owner):
        weights = w_ref[pl.ds(pl.multiple_of(owner * hw, hw), hw), :]
        return jnp.dot(
            rows.reshape(chunk * block_len, hw), weights, preferred_element_type=jnp.float32
        ).reshape(chunk, block_len, -1)

    @pl.loop(0, seqs // chunk)
    def _(i):
        now = pl.ds(i * chunk, chunk)
        acc_ref[now] = term(att_ref[now], me)

    for k in range(1, tp):
        copy(k, lax.rem(me + k, tp)).wait()
        owner = lax.rem(me + tp - k, tp)

        @pl.loop(0, seqs // chunk)
        def _(i):
            now = pl.ds(i * chunk, chunk)
            total = acc_ref[now] + term(held_ref[k - 1, now], owner)
            if k < tp - 1:
                acc_ref[now] = total
            else:
                out_ref[now] = total.astype(out_ref.dtype)


def per_device(n, tp, tokens, w_query, w_key, w_value, w_output, chosen, lengths):
    seqs, block_len, width = tokens.shape
    qw, kw = w_query.shape[1], w_key.shape[1]
    bf16 = jnp.bfloat16
    picked = chosen[:, 0, :]
    vmem = pl.BlockSpec(memory_space=pltpu.VMEM)
    steps = 4
    part = seqs // steps

    def whole(shape):
        return pl.BlockSpec(shape, lambda i: (0,) * len(shape))

    def piece(last):
        return pl.BlockSpec((part, block_len, last), lambda i: (i, 0, 0))

    queries, local, rank, incoming = pl.pallas_call(
        functools.partial(project_kernel, n, steps),
        grid=(steps,),
        out_shape=(
            jax.ShapeDtypeStruct((seqs, block_len, qw), bf16),
            jax.ShapeDtypeStruct((seqs, block_len, 2 * kw), bf16),
            jax.ShapeDtypeStruct((seqs, LANES), jnp.int32),
            jax.ShapeDtypeStruct((n, 8, LANES), jnp.int32),
        ),
        in_specs=[
            piece(width), whole((width, qw)), whole((width, kw)), whole((width, kw)),
            whole(picked.shape), whole((seqs, 1)),
        ],
        out_specs=[piece(qw), piece(2 * kw), whole((seqs, LANES)), whole((n, 8, LANES))],
        scratch_shapes=[
            pltpu.VMEM((n, 8, LANES), jnp.int32),
            pltpu.VMEM((8, LANES), jnp.int32),
            pltpu.SemaphoreType.DMA((n,)),
            pltpu.SemaphoreType.DMA((n,)),
        ],
        compiler_params=pltpu.CompilerParams(
            collective_id=0, has_side_effects=True, vmem_limit_bytes=VMEM_LIMIT
        ),
    )(tokens, w_query, w_key, w_value, picked, lengths[:, None])

    shard = lax.axis_index("kv")
    asked = lax.dynamic_slice_in_dim(incoming[:, :CAP, :], shard, 1, axis=2)
    asked = jnp.clip(asked, 0, seqs - 1).reshape(n * CAP)

    arrived = pl.pallas_call(
        functools.partial(exchange_kernel, n),
        out_shape=jax.ShapeDtypeStruct((n, CAP, block_len, 2 * kw), bf16),
        in_specs=[pl.BlockSpec(memory_space=pltpu.SMEM), vmem],
        out_specs=pl.BlockSpec(memory_space=pl.ANY),
        scratch_shapes=[
            pltpu.VMEM((n, CAP, block_len, 2 * kw), bf16),
            pltpu.SemaphoreType.DMA((n,)),
            pltpu.SemaphoreType.DMA((n,)),
        ],
        compiler_params=pltpu.CompilerParams(
            collective_id=1, has_side_effects=True, vmem_limit_bytes=VMEM_LIMIT
        ),
    )(asked, local)

    w = min(LANES, kw)
    tiles = kw // w
    rows = (w // HEAD_DIM) * (HEADS // KV_HEADS) * block_len
    keep = min(picked.shape[1], n)

    def seq_spec(last):
        return pl.BlockSpec((1, block_len, last), lambda i, *_: (i, 0, 0))

    attended = pl.pallas_call(
        attend_kernel,
        out_shape=jax.ShapeDtypeStruct((seqs, block_len, qw), bf16),
        grid_spec=pltpu.PrefetchScalarGridSpec(
            num_scalar_prefetch=3,
            grid=(seqs,),
            in_specs=[
                seq_spec(qw),
                seq_spec(2 * kw),
                pl.BlockSpec(arrived.shape, lambda i, *_: (0, 0, 0, 0)),
            ],
            out_specs=seq_spec(qw),
            scratch_shapes=[
                pltpu.VMEM((tiles, rows, w), bf16),
                pltpu.VMEM((keep, tiles, rows, block_len), jnp.float32),
                pltpu.VMEM((tiles, rows, block_len), jnp.float32),
                pltpu.VMEM((tiles, rows, block_len), jnp.float32),
                pltpu.VMEM((tiles, rows, w), jnp.float32),
            ],
        ),
        compiler_params=pltpu.CompilerParams(vmem_limit_bytes=VMEM_LIMIT),
    )(lengths, picked, rank, queries, local, arrived)

    out_cols = w_output.shape[1]
    return pl.pallas_call(
        functools.partial(mix_kernel, tp),
        out_shape=jax.ShapeDtypeStruct((seqs, block_len, out_cols), bf16),
        in_specs=[vmem, vmem],
        out_specs=vmem,
        scratch_shapes=[
            pltpu.VMEM((tp - 1, seqs, block_len, qw), bf16),
            pltpu.VMEM((seqs, block_len, out_cols), jnp.float32),
            pltpu.SemaphoreType.DMA((tp - 1,)),
            pltpu.SemaphoreType.DMA((tp - 1,)),
        ],
        compiler_params=pltpu.CompilerParams(
            collective_id=2, has_side_effects=True, vmem_limit_bytes=VMEM_LIMIT
        ),
    )(attended, w_output)


def solution(mesh):
    return jax.shard_map(
        functools.partial(per_device, mesh.shape["kv"], mesh.shape["tp"]),
        mesh=mesh,
        in_specs=(
            P(None, "kv", None),
            P(None, "tp"),
            P(None, "tp"),
            P(None, "tp"),
            P(None, "tp"),
            P(None, "kv", None),
            P(),
        ),
        out_specs=P(None, "kv", "tp"),
        check_vma=False,
    )
```

```python
import functools

import jax
import jax.numpy as jnp
from jax import lax
from jax.experimental import pallas as pl
from jax.experimental.pallas import tpu as pltpu
from jax.sharding import PartitionSpec as P

HEADS = 16
KV_HEADS = 8
HEAD_DIM = 64
LANES = 128
MESH = pl.DeviceIdType.MESH
VMEM_LIMIT = 60 * 1024 * 1024


def block_bound(rank, n):
    return n if rank == 0 else min(n, -(-7 * n // (4 * rank)))


def place(rank, head, seqs, heads):
    half = seqs // 2
    spread = max(heads // 2, 1)
    if rank < half:
        return head * half + rank, 0
    return (head % spread) * half + rank - half, 1 + head // spread


def slot_count(heads):
    spread = max(heads // 2, 1)
    return 1 + -(-heads // spread)


def ranks_of(len_ref, seqs):
    lens = [len_ref[s] for s in range(seqs)]
    ranks = []
    for s in range(seqs):
        rank = jnp.int32(0)
        for o in range(seqs):
            if o != s:
                before = lens[o] >= lens[s] if o < s else lens[o] > lens[s]
                rank = rank + before.astype(jnp.int32)
        ranks.append(rank)
    return ranks


def with_rank(ranks, k):
    found = jnp.int32(0)
    for s in range(len(ranks)):
        found = found + jnp.where(ranks[s] == k, s, 0)
    return found


def greet(axis, me, n):
    barrier = pltpu.get_barrier_semaphore()
    for k in range(1, n):
        pl.semaphore_signal(
            barrier, inc=1, device_id={axis: lax.rem(me + k, n)}, device_id_type=MESH
        )
    return barrier


def project_kernel(
    n, steps, x_ref, wq_ref, wk_ref, wv_ref, chosen_ref,
    local_ref, got_ref, incoming_ref, req_ref, send_sem, recv_sem,
):
    step = pl.program_id(0)
    me = lax.axis_index("kv")
    seqs, slots = chosen_ref.shape
    seqs_now, block_len, width = x_ref.shape

    def list_copy(dest, slot, k=0):
        return pltpu.make_async_remote_copy(
            src_ref=req_ref,
            dst_ref=incoming_ref.at[slot],
            send_sem=send_sem.at[k],
            recv_sem=recv_sem.at[slot],
            device_id={"kv": dest},
            device_id_type=MESH,
        )

    @pl.when(step == 0)
    def _():
        greet("kv", me, n)
        fill = jnp.full((seqs, LANES - slots), -1, jnp.int32)
        lists = jnp.concatenate([chosen_ref[...], fill], axis=1)
        req_ref[...] = lists
        incoming_ref[me] = lists

    rows = x_ref[...].reshape(seqs_now * block_len, width)
    scale = HEAD_DIM ** (-0.5)

    def project(w_ref):
        out = jnp.dot(rows, w_ref[...], preferred_element_type=jnp.float32).astype(jnp.bfloat16)
        return out.reshape(seqs_now, block_len, -1)

    q = project(wq_ref) * jnp.bfloat16(scale)
    k, v = project(wk_ref), project(wv_ref)
    qw = HEAD_DIM * (HEADS // KV_HEADS)
    for g in range(local_ref.shape[1]):
        at = slice(g * HEAD_DIM, (g + 1) * HEAD_DIM)
        local_ref[:, g, :, :qw] = q[:, :, g * qw : (g + 1) * qw]
        local_ref[:, g, :, qw:] = jnp.concatenate([k[:, :, at], v[:, :, at]], axis=2)

    @pl.when(step == 0)
    def _():
        pl.semaphore_wait(pltpu.get_barrier_semaphore(), n - 1)
        for j in range(1, n):
            list_copy(lax.rem(me + j, n), me, j).start()

    @pl.when(step == steps - 1)
    def _():
        for j in range(1, n):
            list_copy(lax.rem(me + j, n), me, j).wait_send()
        for j in range(1, n):
            other = lax.rem(me + j, n)
            list_copy(other, other).wait_recv()
        got_ref[...] = incoming_ref[...]


def exchange_kernel(n, len_ref, local_ref, arrived_ref, pack_ref, send_sem, recv_sem, own_sem):
    me = lax.axis_index("kv")
    seqs, heads = local_ref.shape[:2]
    barrier = greet("kv", me, n)
    ranks = ranks_of(len_ref, seqs)
    units = [(k, g) for k in range(seqs) for g in range(heads)]
    for k in range(seqs):
        s = with_rank(ranks, k)
        for g in range(heads):
            pack_ref[k, g] = local_ref[s, g]
    pl.semaphore_wait(barrier, n - 1)

    def copy(k, g, dest, slot, source):
        return pltpu.make_async_remote_copy(
            src_ref=pack_ref.at[k, g],
            dst_ref=arrived_ref.at[slot, source],
            send_sem=send_sem.at[k, g],
            recv_sem=recv_sem.at[slot, source],
            device_id={"kv": dest},
            device_id_type=MESH,
        )

    def own_copy(k, g, slot):
        return pltpu.make_async_copy(pack_ref.at[k, g], arrived_ref.at[slot, me], own_sem.at[slot])

    for k, g in units:
        owner, slot = place(k, g, seqs, heads)
        sends = me < block_bound(k, n)

        @pl.when(sends & (me != owner))
        def _():
            copy(k, g, owner, slot, me).start()

        @pl.when(sends & (me == owner))
        def _():
            own_copy(k, g, slot).start()

    for k, g in units:
        owner, slot = place(k, g, seqs, heads)
        bound = block_bound(k, n)

        @pl.when((me < bound) & (me != owner))
        def _():
            copy(k, g, owner, slot, me).wait_send()

        @pl.when((me < bound) & (me == owner))
        def _():
            own_copy(k, g, slot).wait()

        @pl.when(me == owner)
        def _():
            @pl.loop(0, bound)
            def _(b):
                @pl.when(b != me)
                def _():
                    copy(k, g, b, slot, b).wait_recv()


def attend_kernel(seqs, heads, sel, n, len_ref, pick_ref, arr_ref, out_ref):
    u = pl.program_id(0)
    me = lax.axis_index("kv")
    block_len = arr_ref.shape[2]
    half = seqs // 2
    group = HEADS // KV_HEADS
    qw = HEAD_DIM * group
    rows = group * block_len
    many = jnp.where(u == 0, heads, max(heads // 2, 1)) * half
    rank = lax.rem(me, half) + jnp.where(u == 0, 0, half)
    s = with_rank(ranks_of(len_ref, seqs), rank)
    length = jnp.where(me < many, len_ref[s], 0)
    live = (length + block_len - 1) // block_len
    unroll = 4
    key_at = lax.broadcasted_iota(jnp.int32, (group, block_len, block_len), 2)
    row_at = lax.broadcasted_iota(jnp.int32, (group, block_len, block_len), 1)
    causal = (key_at <= row_at).reshape(rows, block_len)
    zero = jnp.zeros((block_len, HEAD_DIM), jnp.bfloat16)

    @pl.loop(0, live)
    def _(b):
        base = (b * seqs + s) * sel
        count = jnp.int32(0)
        for j in range(min(sel, n)):
            count = count + (pick_ref[base + j] >= 0).astype(jnp.int32)
        q = arr_ref[0, b, :, :qw]
        qs = jnp.concatenate(
            [
                jnp.concatenate([q[:, h * HEAD_DIM : (h + 1) * HEAD_DIM], zero], axis=1)
                for h in range(group)
            ],
            axis=0,
        )

        def chunk(j0, first):
            blocks, scores = [], []
            for i in range(unroll):
                j = j0 + i
                valid = j < count
                c = jnp.where(valid, pick_ref[base + jnp.minimum(j, sel - 1)], b)
                kv = arr_ref[0, c, :, qw:]
                score = lax.dot_general(
                    qs, kv, (((1,), (1,)), ((), ())), preferred_element_type=jnp.float32
                )
                if first and i == 0:
                    score = jnp.where(causal, score, -1e30)
                else:
                    score = jnp.where(valid, score, -1e30)
                blocks.append(kv)
                scores.append(score)
            top = functools.reduce(jnp.maximum, scores)
            return blocks, scores, jnp.max(top, axis=1, keepdims=True)

        def weigh(blocks, scores, top):
            total, acc = None, None
            for kv, score in zip(blocks, scores):
                p = jnp.exp(score - top)
                got = jnp.dot(p.astype(jnp.bfloat16), kv, preferred_element_type=jnp.float32)
                total = p if total is None else total + p
                acc = got if acc is None else acc + got
            return jnp.sum(total, axis=1, keepdims=True), acc

        blocks, scores, top = chunk(jnp.int32(0), True)
        total, acc = weigh(blocks, scores, top)

        def more(i, carry):
            old, total, acc = carry
            blocks, scores, top = chunk(i * unroll, False)
            top = jnp.maximum(old, top)
            keep = jnp.exp(old - top)
            add, got = weigh(blocks, scores, top)
            return top, total * keep + add, acc * keep + got

        _, total, acc = lax.fori_loop(1, (count + unroll - 1) // unroll, more, (top, total, acc))
        done = acc / total
        parts = [
            done[h * block_len : (h + 1) * block_len, HEAD_DIM : 2 * HEAD_DIM] for h in range(group)
        ]
        done = jnp.concatenate(parts, axis=1)
        at = b * block_len + lax.broadcasted_iota(jnp.int32, done.shape, 0)
        out_ref[0, b] = jnp.where(at < length, done, 0.0).astype(out_ref.dtype)

    @pl.loop(live, n)
    def _(b):
        out_ref[0, b] = jnp.zeros(out_ref.shape[2:], out_ref.dtype)


def mix_kernel(
    n, tp, seqs, heads, len_ref, att_ref, w_ref, out_ref,
    back_ref, held_ref, send_sem, recv_sem, tp_send, tp_recv,
):
    me, my_tp = lax.axis_index("kv"), lax.axis_index("tp")
    block_len, qw = att_ref.shape[2:]
    hw = heads * qw
    pair = 2
    greet("kv", me, n)
    barrier = greet("tp", my_tp, tp)
    pl.semaphore_wait(barrier, n - 1 + tp - 1)
    units = [(k, g) for k in range(seqs) for g in range(heads)]

    def back_copy(k, g, slot, b):
        return pltpu.make_async_remote_copy(
            src_ref=att_ref.at[slot, b],
            dst_ref=back_ref.at[k, g],
            send_sem=send_sem.at[slot, b],
            recv_sem=recv_sem.at[k, g],
            device_id={"kv": b},
            device_id_type=MESH,
        )

    def tp_copy(k, dest):
        return pltpu.make_async_remote_copy(
            src_ref=back_ref,
            dst_ref=held_ref.at[k - 1],
            send_sem=tp_send.at[k - 1],
            recv_sem=tp_recv.at[k - 1],
            device_id={"tp": dest},
            device_id_type=MESH,
        )

    for k, g in units:
        owner, slot = place(k, g, seqs, heads)
        bound = block_bound(k, n)

        @pl.when(me == owner)
        def _():
            @pl.loop(0, bound)
            def _(b):
                @pl.when(b != me)
                def _():
                    back_copy(k, g, slot, b).start()

        @pl.when((me == owner) & (me < bound))
        def _():
            back_ref[k, g] = att_ref[slot, me]

        @pl.when(me >= bound)
        def _():
            back_ref[k, g] = jnp.zeros((block_len, qw), back_ref.dtype)

    ranks = ranks_of(len_ref, seqs)
    for k, g in units:
        owner, slot = place(k, g, seqs, heads)
        bound = block_bound(k, n)

        @pl.when((me < bound) & (me != owner))
        def _():
            back_copy(k, g, slot, owner).wait_recv()

    for k in range(1, tp):
        tp_copy(k, lax.rem(my_tp + k, tp)).start()

    for k, g in units:
        owner, slot = place(k, g, seqs, heads)

        @pl.when(me == owner)
        def _():
            @pl.loop(0, block_bound(k, n))
            def _(b):
                @pl.when(b != me)
                def _():
                    back_copy(k, g, slot, b).wait_send()

    def term(i, source, owner):
        rows = jnp.concatenate(
            [
                jnp.concatenate([source[ranks[i * pair + p], g] for g in range(heads)], axis=1)
                for p in range(pair)
            ],
            axis=0,
        )
        weights = w_ref[pl.ds(pl.multiple_of(owner * hw, hw), hw), :]
        return jnp.dot(rows, weights, preferred_element_type=jnp.float32)

    totals = [term(i, back_ref, my_tp) for i in range(seqs // pair)]
    for k in range(1, tp):
        tp_copy(k, lax.rem(my_tp + k, tp)).wait()
        owner = lax.rem(my_tp + tp - k, tp)
        totals = [t + term(i, held_ref.at[k - 1], owner) for i, t in enumerate(totals)]
    for i, total in enumerate(totals):
        out_ref[i * pair : (i + 1) * pair] = total.reshape(pair, block_len, -1).astype(out_ref.dtype)


def per_device(n, tp, tokens, w_query, w_key, w_value, w_output, chosen, lengths):
    seqs, block_len, width = tokens.shape
    qw, kw = w_query.shape[1], w_key.shape[1]
    heads = kw // HEAD_DIM
    group = HEADS // KV_HEADS
    unit = HEAD_DIM * (group + 2)
    slots = slot_count(heads)
    sel = chosen.shape[2]
    bf16 = jnp.bfloat16
    picked = chosen[:, 0, :]
    vmem = pl.BlockSpec(memory_space=pltpu.VMEM)
    smem = pl.BlockSpec(memory_space=pltpu.SMEM)
    steps = 4
    part = seqs // steps

    def whole(shape):
        return pl.BlockSpec(shape, lambda i: (0,) * len(shape))

    local, lists = pl.pallas_call(
        functools.partial(project_kernel, n, steps),
        grid=(steps,),
        out_shape=(
            jax.ShapeDtypeStruct((seqs, heads, block_len, unit), bf16),
            jax.ShapeDtypeStruct((n, seqs, LANES), jnp.int32),
        ),
        in_specs=[
            pl.BlockSpec((part, block_len, width), lambda i: (i, 0, 0)),
            whole((width, qw)), whole((width, kw)), whole((width, kw)), whole(picked.shape),
        ],
        out_specs=[
            pl.BlockSpec((part, heads, block_len, unit), lambda i: (i, 0, 0, 0)),
            whole((n, seqs, LANES)),
        ],
        scratch_shapes=[
            pltpu.VMEM((n, seqs, LANES), jnp.int32),
            pltpu.VMEM((seqs, LANES), jnp.int32),
            pltpu.SemaphoreType.DMA((n,)),
            pltpu.SemaphoreType.DMA((n,)),
        ],
        compiler_params=pltpu.CompilerParams(
            collective_id=0, has_side_effects=True, vmem_limit_bytes=VMEM_LIMIT
        ),
    )(tokens, w_query, w_key, w_value, picked)

    arrived = pl.pallas_call(
        functools.partial(exchange_kernel, n),
        out_shape=jax.ShapeDtypeStruct((slots, n, block_len, unit), bf16),
        in_specs=[smem, vmem],
        out_specs=pl.BlockSpec(memory_space=pl.ANY),
        scratch_shapes=[
            pltpu.VMEM((seqs, heads, block_len, unit), bf16),
            pltpu.SemaphoreType.DMA((seqs, heads)),
            pltpu.SemaphoreType.DMA((slots, n)),
            pltpu.SemaphoreType.DMA((slots,)),
        ],
        compiler_params=pltpu.CompilerParams(
            collective_id=1, has_side_effects=True, vmem_limit_bytes=VMEM_LIMIT
        ),
    )(lengths, local)

    attended = pl.pallas_call(
        functools.partial(attend_kernel, seqs, heads, sel, n),
        out_shape=jax.ShapeDtypeStruct((slots, n, block_len, HEAD_DIM * group), bf16),
        grid_spec=pltpu.PrefetchScalarGridSpec(
            num_scalar_prefetch=2,
            grid=(slots,),
            in_specs=[pl.BlockSpec((1, n, block_len, unit), lambda i, *_: (i, 0, 0, 0))],
            out_specs=pl.BlockSpec(
                (1, n, block_len, HEAD_DIM * group), lambda i, *_: (i, 0, 0, 0)
            ),
        ),
        compiler_params=pltpu.CompilerParams(vmem_limit_bytes=VMEM_LIMIT),
    )(lengths, lists[:, :, :sel].reshape(n * seqs * sel), arrived)

    out_cols = w_output.shape[1]
    back = (seqs, heads, block_len, HEAD_DIM * group)
    return pl.pallas_call(
        functools.partial(mix_kernel, n, tp, seqs, heads),
        out_shape=jax.ShapeDtypeStruct((seqs, block_len, out_cols), bf16),
        in_specs=[smem, vmem, vmem],
        out_specs=vmem,
        scratch_shapes=[
            pltpu.VMEM(back, bf16),
            pltpu.VMEM((tp - 1,) + back, bf16),
            pltpu.SemaphoreType.DMA((slots, n)),
            pltpu.SemaphoreType.DMA((seqs, heads)),
            pltpu.SemaphoreType.DMA((tp - 1,)),
            pltpu.SemaphoreType.DMA((tp - 1,)),
        ],
        compiler_params=pltpu.CompilerParams(
            collective_id=2, has_side_effects=True, vmem_limit_bytes=VMEM_LIMIT
        ),
    )(lengths, attended, w_output)


def solution(mesh):
    return jax.shard_map(
        functools.partial(per_device, mesh.shape["kv"], mesh.shape["tp"]),
        mesh=mesh,
        in_specs=(
            P(None, "kv", None),
            P(None, "tp"),
            P(None, "tp"),
            P(None, "tp"),
            P(None, "tp"),
            P(None, "kv", None),
            P(),
        ),
        out_specs=P(None, "kv", "tp"),
        check_vma=False,
    )
```

```python
import functools

import jax
import jax.numpy as jnp
from jax import lax
from jax.experimental import pallas as pl
from jax.experimental.pallas import tpu as pltpu
from jax.sharding import PartitionSpec as P

HEADS = 16
KV_HEADS = 8
HEAD_DIM = 64
LANES = 128
MESH = pl.DeviceIdType.MESH
VMEM_LIMIT = 60 * 1024 * 1024


def block_bound(rank, n):
    return n if rank == 0 else min(n, -(-7 * n // (4 * rank)))


def place(rank, head, seqs, heads):
    half = seqs // 2
    spread = max(heads // 2, 1)
    if rank < half:
        return head * half + rank, 0
    return (head % spread) * half + rank - half, 1 + head // spread


def slot_count(heads):
    spread = max(heads // 2, 1)
    return 1 + -(-heads // spread)


def ranks_of(len_ref, seqs):
    lens = [len_ref[s] for s in range(seqs)]
    ranks = []
    for s in range(seqs):
        rank = jnp.int32(0)
        for o in range(seqs):
            if o != s:
                before = lens[o] >= lens[s] if o < s else lens[o] > lens[s]
                rank = rank + before.astype(jnp.int32)
        ranks.append(rank)
    return ranks


def with_rank(ranks, k):
    found = jnp.int32(0)
    for s in range(len(ranks)):
        found = found + jnp.where(ranks[s] == k, s, 0)
    return found


def greet(axis, me, n):
    barrier = pltpu.get_barrier_semaphore()
    for k in range(1, n):
        pl.semaphore_signal(
            barrier, inc=1, device_id={axis: lax.rem(me + k, n)}, device_id_type=MESH
        )
    return barrier


def project_send_kernel(
    n, x_ref, wq_ref, wk_ref, wv_ref, chosen_ref, len_ref, got_ref, arrived_ref,
    incoming_ref, req_ref, pack_ref, list_send, list_recv, send_sem, recv_sem, own_sem,
):
    me = lax.axis_index("kv")
    seqs, slots = chosen_ref.shape
    heads = pack_ref.shape[1]
    block_len = x_ref.shape[1]
    barrier = greet("kv", me, n)
    ranks = ranks_of(len_ref, seqs)
    units = [(k, g) for k in range(seqs) for g in range(heads)]
    pair = 2
    scale = HEAD_DIM ** (-0.5)
    qw = HEAD_DIM * (HEADS // KV_HEADS)
    fill = jnp.full((seqs, LANES - slots), -1, jnp.int32)
    lists = jnp.concatenate([chosen_ref[...], fill], axis=1)
    req_ref[...] = lists
    incoming_ref[me] = lists

    def list_copy(dest, slot, k=0):
        return pltpu.make_async_remote_copy(
            src_ref=req_ref,
            dst_ref=incoming_ref.at[slot],
            send_sem=list_send.at[k],
            recv_sem=list_recv.at[slot],
            device_id={"kv": dest},
            device_id_type=MESH,
        )

    def copy(k, g, dest, slot, source):
        return pltpu.make_async_remote_copy(
            src_ref=pack_ref.at[k, g],
            dst_ref=arrived_ref.at[slot, source],
            send_sem=send_sem.at[k, g],
            recv_sem=recv_sem.at[slot, source],
            device_id={"kv": dest},
            device_id_type=MESH,
        )

    def own_copy(k, g, slot):
        return pltpu.make_async_copy(pack_ref.at[k, g], arrived_ref.at[slot, me], own_sem.at[slot])

    for first in range(0, seqs, pair):
        rows = jnp.concatenate(
            [x_ref[with_rank(ranks, first + p)] for p in range(pair)], axis=0
        )

        def project(w_ref):
            out = jnp.dot(rows, w_ref[...], preferred_element_type=jnp.float32)
            return out.astype(jnp.bfloat16).reshape(pair, block_len, -1)

        q = project(wq_ref) * jnp.bfloat16(scale)
        keys, values = project(wk_ref), project(wv_ref)
        for p in range(pair):
            for g in range(heads):
                at = slice(g * HEAD_DIM, (g + 1) * HEAD_DIM)
                pack_ref[first + p, g, :, :qw] = q[p, :, g * qw : (g + 1) * qw]
                pack_ref[first + p, g, :, qw:] = jnp.concatenate(
                    [keys[p, :, at], values[p, :, at]], axis=1
                )
        if first == 0:
            pl.semaphore_wait(barrier, n - 1)
        for k, g in units[first * heads : (first + pair) * heads]:
            owner, slot = place(k, g, seqs, heads)
            sends = me < block_bound(k, n)

            @pl.when(sends & (me != owner))
            def _():
                copy(k, g, owner, slot, me).start()

            @pl.when(sends & (me == owner))
            def _():
                own_copy(k, g, slot).start()

        if first == 0:
            for j in range(1, n):
                list_copy(lax.rem(me + j, n), me, j).start()

    for j in range(1, n):
        list_copy(lax.rem(me + j, n), me, j).wait_send()
    for j in range(1, n):
        other = lax.rem(me + j, n)
        list_copy(other, other).wait_recv()
    got_ref[...] = incoming_ref[...]

    for k, g in units:
        owner, slot = place(k, g, seqs, heads)
        bound = block_bound(k, n)

        @pl.when((me < bound) & (me != owner))
        def _():
            copy(k, g, owner, slot, me).wait_send()

        @pl.when((me < bound) & (me == owner))
        def _():
            own_copy(k, g, slot).wait()

        @pl.when(me == owner)
        def _():
            @pl.loop(0, bound)
            def _(b):
                @pl.when(b != me)
                def _():
                    copy(k, g, b, slot, b).wait_recv()


def attend_kernel(seqs, heads, sel, n, len_ref, pick_ref, arr_ref, out_ref):
    u = pl.program_id(0)
    me = lax.axis_index("kv")
    block_len = arr_ref.shape[2]
    half = seqs // 2
    group = HEADS // KV_HEADS
    qw = HEAD_DIM * group
    rows = group * block_len
    many = jnp.where(u == 0, heads, max(heads // 2, 1)) * half
    rank = lax.rem(me, half) + jnp.where(u == 0, 0, half)
    s = with_rank(ranks_of(len_ref, seqs), rank)
    length = jnp.where(me < many, len_ref[s], 0)
    live = (length + block_len - 1) // block_len
    unroll = 4
    key_at = lax.broadcasted_iota(jnp.int32, (group, block_len, block_len), 2)
    row_at = lax.broadcasted_iota(jnp.int32, (group, block_len, block_len), 1)
    causal = (key_at <= row_at).reshape(rows, block_len)
    zero = jnp.zeros((block_len, HEAD_DIM), jnp.bfloat16)

    def chunk(row, j0, first):
        b, base, count, qs = row
        blocks, scores = [], []
        for i in range(unroll):
            j = j0 + i
            valid = j < count
            c = jnp.where(valid, pick_ref[base + jnp.minimum(j, sel - 1)], b)
            kv = arr_ref[0, c, :, qw:]
            score = lax.dot_general(
                qs, kv, (((1,), (1,)), ((), ())), preferred_element_type=jnp.float32
            )
            if first and i == 0:
                score = jnp.where(causal, score, -1e30)
            else:
                score = jnp.where(valid, score, -1e30)
            blocks.append(kv)
            scores.append(score)
        top = functools.reduce(jnp.maximum, scores)
        return blocks, scores, jnp.max(top, axis=1, keepdims=True)

    def weigh(blocks, scores, top):
        total, acc = None, None
        for kv, score in zip(blocks, scores):
            p = jnp.exp(score - top)
            got = jnp.dot(p.astype(jnp.bfloat16), kv, preferred_element_type=jnp.float32)
            total = p if total is None else total + p
            acc = got if acc is None else acc + got
        return jnp.sum(total, axis=1, keepdims=True), acc

    def row_of(b):
        base = (b * seqs + s) * sel
        count = jnp.int32(0)
        for j in range(min(sel, n)):
            count = count + (pick_ref[base + j] >= 0).astype(jnp.int32)
        q = arr_ref[0, b, :, :qw]
        qs = jnp.concatenate(
            [
                jnp.concatenate([q[:, h * HEAD_DIM : (h + 1) * HEAD_DIM], zero], axis=1)
                for h in range(group)
            ],
            axis=0,
        )
        return b, base, count, qs

    @pl.loop(0, (live + 1) // 2)
    def _(i):
        both = [row_of(i), row_of(live - 1 - i)]
        opened = [chunk(row, jnp.int32(0), True) for row in both]
        begun = []
        for blocks, scores, top in opened:
            total, acc = weigh(blocks, scores, top)
            begun.append((top, total, acc))

        def more(at, carry):
            opened = [chunk(row, at * unroll, False) for row in both]
            kept = []
            for (old, total, acc), (blocks, scores, top) in zip(carry, opened):
                top = jnp.maximum(old, top)
                keep = jnp.exp(old - top)
                add, got = weigh(blocks, scores, top)
                kept.append((top, total * keep + add, acc * keep + got))
            return tuple(kept)

        longest = jnp.maximum(both[0][2], both[1][2])
        ended = lax.fori_loop(1, (longest + unroll - 1) // unroll, more, tuple(begun))
        for (b, _, _, _), (_, total, acc) in zip(both, ended):
            done = acc / total
            parts = [
                done[h * block_len : (h + 1) * block_len, HEAD_DIM : 2 * HEAD_DIM]
                for h in range(group)
            ]
            done = jnp.concatenate(parts, axis=1)
            at = b * block_len + lax.broadcasted_iota(jnp.int32, done.shape, 0)
            out_ref[0, b] = jnp.where(at < length, done, 0.0).astype(out_ref.dtype)

    @pl.loop(live, n)
    def _(b):
        out_ref[0, b] = jnp.zeros(out_ref.shape[2:], out_ref.dtype)


def mix_kernel(
    n, tp, seqs, heads, len_ref, att_ref, w_ref, out_ref,
    back_ref, held_ref, send_sem, recv_sem, tp_send, tp_recv,
):
    me, my_tp = lax.axis_index("kv"), lax.axis_index("tp")
    block_len, qw = att_ref.shape[2:]
    hw = heads * qw
    pair = 2
    greet("kv", me, n)
    barrier = greet("tp", my_tp, tp)
    pl.semaphore_wait(barrier, n - 1 + tp - 1)
    units = [(k, g) for k in range(seqs) for g in range(heads)]

    def back_copy(k, g, slot, b):
        return pltpu.make_async_remote_copy(
            src_ref=att_ref.at[slot, b],
            dst_ref=back_ref.at[k, g],
            send_sem=send_sem.at[slot, b],
            recv_sem=recv_sem.at[k, g],
            device_id={"kv": b},
            device_id_type=MESH,
        )

    def tp_copy(k, dest):
        return pltpu.make_async_remote_copy(
            src_ref=back_ref,
            dst_ref=held_ref.at[k - 1],
            send_sem=tp_send.at[k - 1],
            recv_sem=tp_recv.at[k - 1],
            device_id={"tp": dest},
            device_id_type=MESH,
        )

    for k, g in units:
        owner, slot = place(k, g, seqs, heads)
        bound = block_bound(k, n)

        @pl.when(me == owner)
        def _():
            @pl.loop(0, bound)
            def _(b):
                @pl.when(b != me)
                def _():
                    back_copy(k, g, slot, b).start()

        @pl.when((me == owner) & (me < bound))
        def _():
            back_ref[k, g] = att_ref[slot, me]

        @pl.when(me >= bound)
        def _():
            back_ref[k, g] = jnp.zeros((block_len, qw), back_ref.dtype)

    ranks = ranks_of(len_ref, seqs)
    for k, g in units:
        owner, slot = place(k, g, seqs, heads)
        bound = block_bound(k, n)

        @pl.when((me < bound) & (me != owner))
        def _():
            back_copy(k, g, slot, owner).wait_recv()

    for k in range(1, tp):
        tp_copy(k, lax.rem(my_tp + k, tp)).start()

    for k, g in units:
        owner, slot = place(k, g, seqs, heads)

        @pl.when(me == owner)
        def _():
            @pl.loop(0, block_bound(k, n))
            def _(b):
                @pl.when(b != me)
                def _():
                    back_copy(k, g, slot, b).wait_send()

    def term(i, source, owner):
        rows = jnp.concatenate(
            [
                jnp.concatenate([source[ranks[i * pair + p], g] for g in range(heads)], axis=1)
                for p in range(pair)
            ],
            axis=0,
        )
        weights = w_ref[pl.ds(pl.multiple_of(owner * hw, hw), hw), :]
        return jnp.dot(rows, weights, preferred_element_type=jnp.float32)

    totals = [term(i, back_ref, my_tp) for i in range(seqs // pair)]
    for k in range(1, tp):
        tp_copy(k, lax.rem(my_tp + k, tp)).wait()
        owner = lax.rem(my_tp + tp - k, tp)
        totals = [t + term(i, held_ref.at[k - 1], owner) for i, t in enumerate(totals)]
    for i, total in enumerate(totals):
        out_ref[i * pair : (i + 1) * pair] = total.reshape(pair, block_len, -1).astype(out_ref.dtype)


def per_device(n, tp, tokens, w_query, w_key, w_value, w_output, chosen, lengths):
    seqs, block_len, width = tokens.shape
    qw, kw = w_query.shape[1], w_key.shape[1]
    heads = kw // HEAD_DIM
    group = HEADS // KV_HEADS
    unit = HEAD_DIM * (group + 2)
    slots = slot_count(heads)
    sel = chosen.shape[2]
    bf16 = jnp.bfloat16
    picked = chosen[:, 0, :]
    vmem = pl.BlockSpec(memory_space=pltpu.VMEM)
    smem = pl.BlockSpec(memory_space=pltpu.SMEM)
    lists, arrived = pl.pallas_call(
        functools.partial(project_send_kernel, n),
        out_shape=(
            jax.ShapeDtypeStruct((n, seqs, LANES), jnp.int32),
            jax.ShapeDtypeStruct((slots, n, block_len, unit), bf16),
        ),
        in_specs=[vmem, vmem, vmem, vmem, vmem, smem],
        out_specs=[vmem, pl.BlockSpec(memory_space=pl.ANY)],
        scratch_shapes=[
            pltpu.VMEM((n, seqs, LANES), jnp.int32),
            pltpu.VMEM((seqs, LANES), jnp.int32),
            pltpu.VMEM((seqs, heads, block_len, unit), bf16),
            pltpu.SemaphoreType.DMA((n,)),
            pltpu.SemaphoreType.DMA((n,)),
            pltpu.SemaphoreType.DMA((seqs, heads)),
            pltpu.SemaphoreType.DMA((slots, n)),
            pltpu.SemaphoreType.DMA((slots,)),
        ],
        compiler_params=pltpu.CompilerParams(
            collective_id=0, has_side_effects=True, vmem_limit_bytes=VMEM_LIMIT
        ),
    )(tokens, w_query, w_key, w_value, picked, lengths)

    attended = pl.pallas_call(
        functools.partial(attend_kernel, seqs, heads, sel, n),
        out_shape=jax.ShapeDtypeStruct((slots, n, block_len, HEAD_DIM * group), bf16),
        grid_spec=pltpu.PrefetchScalarGridSpec(
            num_scalar_prefetch=2,
            grid=(slots,),
            in_specs=[pl.BlockSpec((1, n, block_len, unit), lambda i, *_: (i, 0, 0, 0))],
            out_specs=pl.BlockSpec(
                (1, n, block_len, HEAD_DIM * group), lambda i, *_: (i, 0, 0, 0)
            ),
        ),
        compiler_params=pltpu.CompilerParams(vmem_limit_bytes=VMEM_LIMIT),
    )(lengths, lists[:, :, :sel].reshape(n * seqs * sel), arrived)

    out_cols = w_output.shape[1]
    back = (seqs, heads, block_len, HEAD_DIM * group)
    return pl.pallas_call(
        functools.partial(mix_kernel, n, tp, seqs, heads),
        out_shape=jax.ShapeDtypeStruct((seqs, block_len, out_cols), bf16),
        in_specs=[smem, vmem, vmem],
        out_specs=vmem,
        scratch_shapes=[
            pltpu.VMEM(back, bf16),
            pltpu.VMEM((tp - 1,) + back, bf16),
            pltpu.SemaphoreType.DMA((slots, n)),
            pltpu.SemaphoreType.DMA((seqs, heads)),
            pltpu.SemaphoreType.DMA((tp - 1,)),
            pltpu.SemaphoreType.DMA((tp - 1,)),
        ],
        compiler_params=pltpu.CompilerParams(
            collective_id=2, has_side_effects=True, vmem_limit_bytes=VMEM_LIMIT
        ),
    )(lengths, attended, w_output)


def solution(mesh):
    return jax.shard_map(
        functools.partial(per_device, mesh.shape["kv"], mesh.shape["tp"]),
        mesh=mesh,
        in_specs=(
            P(None, "kv", None),
            P(None, "tp"),
            P(None, "tp"),
            P(None, "tp"),
            P(None, "tp"),
            P(None, "kv", None),
            P(),
        ),
        out_specs=P(None, "kv", "tp"),
        check_vma=False,
    )
```
